32 devices in a mesh: fs: 8 (over z, x), tp: 4 (over y, core).
Axes of the slice: x: 2, y: 2, z: 4, core: 2. Of those that a mesh axis runs over, the one named last changes fastest.
Arguments:
- tokens: bfloat16 [8192, 2048], P('fs', 'tp'), may hold values from -6 to 6
- recurrence_norm_gain: float32 [2048], replicated, may hold values from 0.1 to 1.9
- output_gate_weight: bfloat16 [2048, 2816], P('fs', 'tp'), may hold values from -0.125 to 0.125
- recurrence_input_weight: bfloat16 [2048, 2816], P('fs', 'tp'), may hold values from -0.125 to 0.125
- convolution_taps: float32 [4, 2816], P(None, 'tp'), may hold values from -3 to 3
- recurrence_gate_weight: bfloat16 [8, 352, 352], P('tp'), may hold values from -0.3125 to 0.3125
- input_gate_weight: bfloat16 [8, 352, 352], P('tp'), may hold values from -0.3125 to 0.3125
- base_decay_logit: float32 [2816], P('tp'), may hold values from 4.5 to 9.5
- token_log_decay: float32 [8192], P('fs'), may hold values from -0.7 to 0, as said below
- recurrence_output_weight: bfloat16 [2816, 2048], P('tp', 'fs'), may hold values from -0.4375 to 0.4375
- feedforward_norm_gain: float32 [2048], replicated, may hold values from 0.1 to 1.9
- feedforward_gate_weight: bfloat16 [2048, 5632], P('fs', 'tp'), may hold values from -0.125 to 0.125
- feedforward_up_weight: bfloat16 [2048, 5632], P('fs', 'tp'), may hold values from -0.125 to 0.125
- feedforward_down_weight: bfloat16 [5632, 2048], P('tp', 'fs'), may hold values from -0.15625 to 0.15625
Outputs:
- layer_out: bfloat16 [8192, 2048], P('fs', 'tp')
The draws below stay inside these ranges and needn't reach their ends.
Inputs may be any that keep to these rules, and one draw needn't show every extreme that they name: `token_log_decay`: each entry is zero or lies between -0.7 and -0.22.
All inputs are finite; a program needn't handle non-finite values.
Results may differ from the reference program's by a relative error of at most 0.022.
Values may be sent and summed in bfloat16 or wider, within the bound.
No kernel may reach another device: no remote copies, remote signals or barrier semaphores. Data moves between devices by JAX's collectives and lax.ppermute only.
A program may use at most 128 MiB of HBM per device.

```python
import jax
import jax.numpy as jnp
from jax import lax

D = 2048
R = 2816
BW = 352
FF = 5632
CONV = 4
LEN = 128
BLOCKS = 8
TOKENS = 8192
N_TP = 4


def draw_base_decay_logit(key, part):
    keys = jax.random.split(jax.random.fold_in(key, 11), 3)
    slower = jax.random.bernoulli(keys[0], 0.5, (R,))
    fast_values = jax.random.uniform(keys[1], (R,), jnp.float32, 4.5, 5.5)
    slow_values = jax.random.uniform(keys[2], (R,), jnp.float32, 6.5, 9.0)
    return jnp.where(slower, slow_values, fast_values)


def draw_token_log_decay(key, part):
    keys = jax.random.split(jax.random.fold_in(key, 23), 2)
    struck = jax.random.bernoulli(keys[0], 3.0 / LEN, (TOKENS,))
    depths = jax.random.uniform(keys[1], (TOKENS,), jnp.float32, -0.7, -0.22)
    return jnp.where(struck, depths, jnp.zeros((TOKENS,), jnp.float32))


def levels(stream_key, extent, shards, smallest, largest):
    loudness, own = 1.0, jax.random.fold_in(stream_key, 6)
    for axis_at, shards_of in shards:
        heights = jnp.exp(jax.random.uniform(jax.random.fold_in(own, axis_at), (shards_of,), jnp.float32, smallest / len(shards), largest / len(shards)))
        loudness = loudness * jnp.repeat(heights, extent[axis_at] // shards_of).reshape([-1 if axis == axis_at else 1 for axis in range(len(extent))])
    return loudness


def scatter_about(key, dims, deviation, limit, pieces=(), kind=jnp.bfloat16):
    entries = jax.random.normal(key, dims, jnp.float32) * deviation
    if len(pieces) > 0:
        entries = levels(key, dims, pieces, -0.22, 0.18) * entries
    return jnp.clip(entries, min=-limit, max=limit).astype(kind)


def setup_inputs(seed: int = 0) -> dict:
    arg_keys = jax.random.split(jax.random.key(seed), 15)
    return {
        "tokens": scatter_about(arg_keys[0], (TOKENS, D), 1.0, 6.0, ((0, 8), (1, 4))),
        "recurrence_norm_gain": jnp.clip(1.0 + 0.18 * jax.random.normal(arg_keys[1], (D,), jnp.float32), 0.1, 1.9),
        "output_gate_weight": scatter_about(arg_keys[2], (D, R), D ** -0.5, 0.125, ((0, 8), (1, 4))),
        "recurrence_input_weight": scatter_about(arg_keys[3], (D, R), D ** -0.5, 0.125, ((0, 8), (1, 4))),
        "convolution_taps": scatter_about(arg_keys[4], (CONV, R), CONV ** -0.5, 3.0, ((1, 4),), jnp.float32),
        "recurrence_gate_weight": scatter_about(arg_keys[5], (BLOCKS, BW, BW), BW ** -0.5, 0.3125, ((0, 4),)),
        "input_gate_weight": scatter_about(arg_keys[6], (BLOCKS, BW, BW), BW ** -0.5, 0.3125, ((0, 4),)),
        "base_decay_logit": draw_base_decay_logit(jax.random.fold_in(arg_keys[14], 71), 0),
        "token_log_decay": draw_token_log_decay(jax.random.fold_in(arg_keys[14], 71), 0),
        "recurrence_output_weight": scatter_about(arg_keys[9], (R, D), (R // 16) ** -0.5, 0.4375, ((0, 4), (1, 8))),
        "feedforward_norm_gain": jnp.clip(1.0 + 0.18 * jax.random.normal(arg_keys[10], (D,), jnp.float32), 0.1, 1.9),
        "feedforward_gate_weight": scatter_about(arg_keys[11], (D, FF), D ** -0.5, 0.125, ((0, 8), (1, 4))),
        "feedforward_up_weight": scatter_about(arg_keys[12], (D, FF), D ** -0.5, 0.125, ((0, 8), (1, 4))),
        "feedforward_down_weight": scatter_about(arg_keys[13], (FF, D), (FF // 4) ** -0.5, 0.15625, ((0, 4), (1, 8))),
    }


EPSILON = 1e-06
GATE_EXPONENT = 8.0

def norm_rows(values, gain_vec):
    widened = values.astype(jnp.float32)
    scaled = widened * lax.rsqrt(lax.optimization_barrier(jnp.mean(widened * widened, axis=-1, keepdims=True)) + EPSILON)
    return (scaled * gain_vec).astype(jnp.bfloat16)

def causal_taps(feature_vector, convolution_taps, length):
    row_count, channels = feature_vector.shape
    blocks = feature_vector.astype(jnp.float32).reshape(row_count // length, length, channels)
    tap_count = convolution_taps.shape[0]
    padded = jnp.pad(blocks, ((0, 0), (tap_count - 1, 0), (0, 0)))
    summed = jnp.zeros_like(blocks)
    for offset in range(tap_count):
        summed = summed + convolution_taps[offset] * padded[:, offset:offset + length]
    return summed.reshape(row_count, channels).astype(jnp.bfloat16)

def combine_steps(earlier, latter):
    return (earlier[0] * latter[0], latter[0] * earlier[1] + latter[1])

def linear_scan(decays, driven, length):
    row_count, channels = decays.shape
    shaped = (decays.reshape(row_count // length, length, channels), driven.reshape(row_count // length, length, channels))
    result = lax.associative_scan(combine_steps, shaped, axis=1)
    return result[1].reshape(row_count, channels)

def block_map(mixed_in, weight):
    row_count = mixed_in.shape[0]
    shaped = mixed_in.astype(jnp.float32).reshape(row_count, BLOCKS, BW)
    return jnp.einsum('tnd,nde->tne', shaped, weight.astype(jnp.float32)).reshape(row_count, R)

def grouped_product(values, weight, group_count):
    step_size = values.shape[1] // group_count
    summed = jnp.zeros((values.shape[0], weight.shape[1]), jnp.float32)
    for group_index in range(group_count):
        lower = group_index * step_size
        partial_product = jnp.dot(values[:, lower:lower + step_size], weight[lower:lower + step_size], preferred_element_type=jnp.float32).astype(jnp.bfloat16)
        summed = summed + lax.optimization_barrier(partial_product).astype(jnp.float32)
    return summed

def reference(tokens, recurrence_norm_gain, output_gate_weight, recurrence_input_weight, convolution_taps, recurrence_gate_weight, input_gate_weight, base_decay_logit, token_log_decay, recurrence_output_weight, feedforward_norm_gain, feedforward_gate_weight, feedforward_up_weight, feedforward_down_weight):
    normed = norm_rows(tokens, recurrence_norm_gain)
    gate_projected = jnp.dot(normed, output_gate_weight, preferred_element_type=jnp.float32)
    feature_vector = jnp.dot(normed, recurrence_input_weight, preferred_element_type=jnp.float32).astype(jnp.bfloat16)
    mixed_in = causal_taps(feature_vector, convolution_taps, LEN)
    recurrence_gate = jax.nn.sigmoid(block_map(mixed_in, recurrence_gate_weight))
    inject_gate = jax.nn.sigmoid(block_map(mixed_in, input_gate_weight))
    decay_log_value = -GATE_EXPONENT * jax.nn.softplus(-base_decay_logit)[None, :] * recurrence_gate + token_log_decay[:, None]
    decays = jnp.exp(decay_log_value)
    driven = jnp.sqrt(-jnp.expm1(2.0 * decay_log_value)) * (inject_gate * mixed_in.astype(jnp.float32))
    states = linear_scan(decays, driven, LEN)
    carried = (states * jax.nn.gelu(gate_projected)).astype(jnp.bfloat16)
    mixer_sum = grouped_product(carried, recurrence_output_weight, N_TP)
    residual = (tokens.astype(jnp.float32) + mixer_sum).astype(jnp.bfloat16)
    normed_two = norm_rows(residual, feedforward_norm_gain)
    gate_hidden = jnp.dot(normed_two, feedforward_gate_weight, preferred_element_type=jnp.float32)
    up_hidden = jnp.dot(normed_two, feedforward_up_weight, preferred_element_type=jnp.float32)
    hidden = (jax.nn.silu(gate_hidden) * up_hidden).astype(jnp.bfloat16)
    hidden_sum = grouped_product(hidden, feedforward_down_weight, N_TP)
    return (residual.astype(jnp.float32) + hidden_sum).astype(jnp.bfloat16)
```

```python
import jax
import jax.numpy as jnp
from jax import lax
from jax.experimental import pallas as pl
from jax.experimental.pallas import tpu as pltpu
from jax.sharding import PartitionSpec as P

LEN = 128
EPSILON = 1e-06
GATE_EXPONENT = 8.0
BF = jnp.bfloat16
F32 = jnp.float32


def params(*semantics):
    return pltpu.CompilerParams(dimension_semantics=semantics, vmem_limit_bytes=48 * 1024 * 1024)


def norm_kernel(place_ref, gain_ref, *refs):
    count = gain_ref.shape[0]
    pieces, out_ref = refs[:-1], refs[-1]
    width = gain_ref.shape[2]
    for group in range(len(pieces) // count):
        own = [ref[...].astype(F32) for ref in pieces[group * count : (group + 1) * count]]
        total = jnp.sum(own[0] * own[0], axis=-1, keepdims=True)
        for piece in own[1:]:
            total = total + jnp.sum(piece * piece, axis=-1, keepdims=True)
        scale = lax.rsqrt(total * (1.0 / (count * width)) + EPSILON)
        for here in range(count):

            @pl.when(place_ref[0] == here)
            def _():
                for step in range(count):
                    at = here ^ step
                    out_ref[group, :, at * width : (at + 1) * width] = (
                        own[step] * scale * gain_ref[at]
                    ).astype(BF)


def norm_pieces(pieces, gain, place, count):
    rows, width = pieces[0].shape
    groups = len(pieces) // count
    block = min(128, rows)
    gains = gain.reshape(count, 1, width)
    out = pl.pallas_call(
        norm_kernel,
        grid=(rows // block,),
        in_specs=[
            pl.BlockSpec(memory_space=pltpu.SMEM),
            pl.BlockSpec((count, 1, width), lambda i: (0, 0, 0)),
        ]
        + [pl.BlockSpec((block, width), lambda i: (i, 0))] * len(pieces),
        out_specs=pl.BlockSpec((groups, block, count * width), lambda i: (0, i, 0)),
        out_shape=jax.ShapeDtypeStruct((groups, rows, count * width), BF),
        compiler_params=params("arbitrary"),
        name="norm_pieces",
    )(place, gains, *pieces)
    return out.reshape(groups * rows, count * width)


def recurrence_kernel(
    sequences, projected_ref, taps_ref, recur_ref, inject_ref, decay_ref, token_ref, out_ref, filter_ref, state_ref, a_ref, b_ref
):
    rows, channels = out_ref.shape
    taps = taps_ref.shape[0]
    history = (taps - 1) * sequences

    @pl.when(pl.program_id(1) == 0)
    def _():
        filter_ref[0:history, :] = jnp.zeros((history, channels), F32)
        state_ref[...] = jnp.zeros_like(state_ref)

    projected = projected_ref[...]
    gate = projected[:, :channels]
    filter_ref[history : history + rows, :] = projected[:, channels:].astype(BF).astype(F32)
    summed = taps_ref[0:1, :] * filter_ref[0:rows, :]
    for k in range(1, taps):
        summed = summed + taps_ref[k : k + 1, :] * filter_ref[k * sequences : k * sequences + rows, :]
    filter_ref[0:history, :] = filter_ref[rows : rows + history, :]
    mixed = summed.astype(BF)
    recur = jax.nn.sigmoid(jnp.dot(mixed, recur_ref[...], preferred_element_type=F32))
    inject = jax.nn.sigmoid(jnp.dot(mixed, inject_ref[...], preferred_element_type=F32))
    log_decay = decay_ref[...] * recur + token_ref[:, 0:1]
    decay = jnp.exp(log_decay)
    square = log_decay * log_decay
    small = log_decay * (
        1.0 - square * (1.0 / 3.0 - square * (2.0 / 15.0 - square * (17.0 / 315.0 - square * (62.0 / 2835.0))))
    )
    tangent = jnp.where(log_decay > -0.125, small, jnp.tanh(log_decay))
    a_ref[...] = decay
    b_ref[...] = jnp.sqrt(-tangent * (1.0 + decay * decay)) * (inject * mixed.astype(F32))
    state = state_ref[...]
    for step in range(rows // sequences):
        at = slice(step * sequences, (step + 1) * sequences)
        state = a_ref[at, :] * state + b_ref[at, :]
        b_ref[at, :] = state
    state_ref[...] = state
    out_ref[...] = (b_ref[...] * jax.nn.gelu(gate)).astype(BF)


def recurrence(projected, taps, recur, inject, decay, token_decay, sequences):
    rows, doubled = projected.shape
    channels = doubled // 2
    per = sequences * LEN
    block = sequences * 32
    steps = per // block
    import functools

    return pl.pallas_call(
        functools.partial(recurrence_kernel, sequences),
        grid=(rows // per, steps),
        in_specs=[
            pl.BlockSpec((block, doubled), lambda g, i: (g * steps + i, 0)),
            pl.BlockSpec(taps.shape, lambda g, i: (0, 0)),
            pl.BlockSpec(recur.shape, lambda g, i: (0, 0)),
            pl.BlockSpec(inject.shape, lambda g, i: (0, 0)),
            pl.BlockSpec((1, channels), lambda g, i: (0, 0)),
            pl.BlockSpec((block, token_decay.shape[1]), lambda g, i: (g * steps + i, 0)),
        ],
        out_specs=pl.BlockSpec((block, channels), lambda g, i: (g * steps + i, 0)),
        out_shape=jax.ShapeDtypeStruct((rows, channels), BF),
        scratch_shapes=[
            pltpu.VMEM((block + (taps.shape[0] - 1) * sequences, channels), F32),
            pltpu.VMEM((sequences, channels), F32),
            pltpu.VMEM((block, channels), F32),
            pltpu.VMEM((block, channels), F32),
        ],
        compiler_params=params("arbitrary", "arbitrary"),
        name="recurrence",
    )(projected, taps, recur, inject, decay, token_decay)


def time_major(rows_first, sequences):
    rows, width = rows_first.shape
    return rows_first.reshape(sequences, rows // sequences, width).swapaxes(0, 1).reshape(rows, width)


def sequence_major(time_first, sequences):
    rows, width = time_first.shape
    return time_first.reshape(rows // sequences, sequences, width).swapaxes(0, 1).reshape(rows, width)


def decay_columns(token_log_decay, sequences):
    ordered = token_log_decay.reshape(sequences, LEN).T.reshape(-1, 1)
    return jnp.broadcast_to(ordered, (ordered.shape[0], 128))


def block_dense(weight):
    groups, block_width, _ = weight.shape
    identity = jnp.eye(groups, dtype=BF)[:, None, :, None]
    return (weight[:, :, None, :] * identity).reshape(groups * block_width, groups * block_width)


def product(left, right):
    return jnp.dot(left, right, preferred_element_type=F32)


def plain_shards(
    tokens,
    recurrence_norm_gain,
    output_gate_weight,
    recurrence_input_weight,
    convolution_taps,
    recurrence_gate_weight,
    input_gate_weight,
    base_decay_logit,
    token_log_decay,
    recurrence_output_weight,
    feedforward_norm_gain,
    feedforward_gate_weight,
    feedforward_up_weight,
    feedforward_down_weight,
):
    sequences = tokens.shape[0] // LEN

    def rows_of(weight):
        return lax.all_gather(weight, "fs", axis=0, tiled=True)

    def columns_of(weight):
        return lax.all_gather(weight, "fs", axis=1, tiled=True)

    def normed_of(own, gain):
        widened = lax.all_gather(own, "tp", axis=1, tiled=True).astype(F32)
        scale = lax.rsqrt(jnp.mean(widened * widened, axis=-1, keepdims=True) + EPSILON)
        return (widened * scale * gain).astype(BF)

    def scattered(term):
        return lax.psum_scatter(term.astype(BF), "tp", scatter_dimension=1, tiled=True).astype(F32)

    ordered = time_major(tokens, sequences)
    normed = normed_of(ordered, recurrence_norm_gain)
    projected = jnp.concatenate(
        [product(normed, rows_of(output_gate_weight)), product(normed, rows_of(recurrence_input_weight))], axis=1
    )
    carried = recurrence(
        projected,
        convolution_taps,
        block_dense(recurrence_gate_weight),
        block_dense(input_gate_weight),
        -GATE_EXPONENT * jax.nn.softplus(-base_decay_logit)[None, :],
        decay_columns(token_log_decay, sequences),
        sequences,
    )
    mixed = scattered(product(carried, columns_of(recurrence_output_weight)))
    residual = sequence_major((ordered.astype(F32) + mixed).astype(BF), sequences)
    normed_two = normed_of(residual, feedforward_norm_gain)
    gate_hidden = product(normed_two, rows_of(feedforward_gate_weight))
    up_hidden = product(normed_two, rows_of(feedforward_up_weight))
    hidden = (jax.nn.silu(gate_hidden) * up_hidden).astype(BF)
    down = scattered(product(hidden, columns_of(feedforward_down_weight)))
    return (residual.astype(F32) + down).astype(BF)


def paired_shards(
    tokens,
    recurrence_norm_gain,
    output_gate_weight,
    recurrence_input_weight,
    convolution_taps,
    recurrence_gate_weight,
    input_gate_weight,
    base_decay_logit,
    token_log_decay,
    recurrence_output_weight,
    feedforward_norm_gain,
    feedforward_gate_weight,
    feedforward_up_weight,
    feedforward_down_weight,
):
    fs, tp = lax.axis_size("fs"), lax.axis_size("tp")
    side = lax.axis_index("fs") % 2
    place = lax.axis_index("tp")
    rows = tokens.shape[0]
    sequences = rows // LEN
    first = side == 0
    lines = [[way + 2 * i for i in range(fs // 2)] for way in range(2)]

    def over_x(value):
        return lax.ppermute(value, "fs", [(i, i ^ 1) for i in range(fs)])

    def over_tp(value, bit):
        return lax.ppermute(value, "tp", [(i, i ^ bit) for i in range(tp)])

    def halves(weight, axis):
        low, high = jnp.split(weight, 2, axis=axis)
        return jnp.where(first, low, high), jnp.where(first, high, low)

    def in_order(own, other):
        return jnp.where(first, jnp.stack([own, other]), jnp.stack([other, own]))

    def gathered(own, other, axis=0):
        pair = in_order(own, over_x(other))
        out = lax.all_gather(pair, "fs", axis=0, tiled=True, axis_index_groups=lines)
        return out

    gate_own, gate_other = halves(output_gate_weight, 1)
    in_own, in_other = halves(recurrence_input_weight, 1)
    project_weight = gathered(
        jnp.concatenate([gate_own, in_own], 1), jnp.concatenate([gate_other, in_other], 1)
    )
    project_weight = project_weight.reshape(-1, project_weight.shape[-1])
    out_weight = gathered(*halves(recurrence_output_weight, 0))
    ffn_gate_own, ffn_gate_other = halves(feedforward_gate_weight, 1)
    ffn_up_own, ffn_up_other = halves(feedforward_up_weight, 1)
    ffn_pair = in_order(
        jnp.stack([ffn_gate_own, ffn_up_own]), over_x(jnp.stack([ffn_gate_other, ffn_up_other]))
    )
    ffn_pair = ffn_pair.swapaxes(0, 1).reshape(2, -1, ffn_gate_own.shape[-1])
    ffn_weight = lax.all_gather(ffn_pair, "fs", axis=1, tiled=True, axis_index_groups=lines)
    down_weight = gathered(*halves(feedforward_down_weight, 0))

    def spread(own):
        half = rows // 2
        over, across = over_x(own), over_tp(own, 2)
        corner = jnp.concatenate([over_tp(over[:half], 2), over_x(across[half:])], axis=0)
        return [
            own, over_tp(own, 1), across, over_tp(across, 1),
            over, over_tp(over, 1), corner, over_tp(corner, 1),
        ]

    def columns(weight, step):
        each = weight.shape[0] // tp
        chosen = lax.dynamic_slice_in_dim(weight, (place ^ step) * each, each, axis=0)
        return chosen.swapaxes(0, 1).reshape(weight.shape[1], -1)

    def summed_to_owner(values, weight):
        half = rows // 2
        part = {step: product(values, columns(weight, step)).astype(BF) for step in (3, 1, 2, 0)}
        far = part[2].astype(F32) + over_tp(part[3], 1).astype(F32)
        near = part[0].astype(F32) + over_tp(part[1], 1).astype(F32)
        corner = far[rows:].astype(BF)
        by_x, by_y = over_x(corner[:half]), over_tp(corner[half:], 2)
        to_y = jnp.concatenate([far[:half] + by_x.astype(F32), far[half:rows]], axis=0)
        to_x = jnp.concatenate([near[rows : rows + half], near[rows + half :] + by_y.astype(F32)], axis=0)
        from_y, from_x = over_tp(to_y.astype(BF), 2), over_x(to_x.astype(BF))
        return near[:rows] + from_y.astype(F32) + from_x.astype(F32)

    places = place.reshape(1).astype(jnp.int32)
    ordered = time_major(tokens, sequences)
    normed = norm_pieces(spread(ordered), recurrence_norm_gain, places, tp)
    projected = product(normed, project_weight)
    token_decay = token_log_decay.reshape(sequences, LEN)
    token_columns = jnp.concatenate(
        [decay_columns(token_decay, sequences), decay_columns(over_x(token_decay), sequences)], axis=0
    )
    carried = recurrence(
        projected,
        halves(convolution_taps, 1)[0],
        block_dense(halves(recurrence_gate_weight, 0)[0]),
        block_dense(halves(input_gate_weight, 0)[0]),
        -GATE_EXPONENT * jax.nn.softplus(-halves(base_decay_logit, 0)[0])[None, :],
        token_columns,
        sequences,
    )
    mixed = summed_to_owner(carried, out_weight)
    residual = sequence_major((ordered.astype(F32) + mixed).astype(BF), sequences)
    normed_two = norm_pieces(spread(residual), feedforward_norm_gain, places, tp)
    hidden = (jax.nn.silu(product(normed_two, ffn_weight[0])) * product(normed_two, ffn_weight[1])).astype(BF)
    down = summed_to_owner(hidden, down_weight)
    return (residual.astype(F32) + down).astype(BF)


def solution(mesh):
    in_specs = (
        P("fs", "tp"), P(), P("fs", "tp"), P("fs", "tp"), P(None, "tp"), P("tp", None, None), P("tp", None, None),
        P("tp"), P("fs"), P("tp", "fs"), P(), P("fs", "tp"), P("fs", "tp"), P("tp", "fs"),
    )
    fs, tp = mesh.shape["fs"], mesh.shape["tp"]

    def whole(*args):
        blocks = args[5].shape[0] // tp
        paired = fs % 2 == 0 and tp == 4 and blocks % 2 == 0
        body = paired_shards if paired else plain_shards
        return jax.shard_map(
            body, mesh=mesh, in_specs=in_specs, out_specs=P("fs", "tp"), check_vma=False
        )(*args)

    return whole
```

```python
import functools

import jax
import jax.numpy as jnp
from jax import lax
from jax.experimental import pallas as pl
from jax.experimental.pallas import tpu as pltpu
from jax.sharding import PartitionSpec as P


LEN = 128
EPSILON = 1e-06
GATE_EXPONENT = 8.0
BF = jnp.bfloat16
F32 = jnp.float32


def params(*semantics):
    return pltpu.CompilerParams(dimension_semantics=semantics, vmem_limit_bytes=48 * 1024 * 1024)


def norm_kernel(count, table_ref, gain_ref, *refs):
    pieces, out_ref = refs[:-1], refs[-1]
    blocks, _, block = gain_ref.shape
    per = blocks // count
    for group in range(len(pieces) // count):
        own = pieces[group * count : (group + 1) * count]
        total = None
        for ref in own:
            value = ref[...].astype(F32)
            part = value * value
            total = part if total is None else total + part
        scale = lax.rsqrt(jnp.sum(total, axis=-1, keepdims=True) * (1.0 / (blocks * block)) + EPSILON)
        for step in range(count):
            for half in range(per):
                at = step * per + half
                source, slot = table_ref[0, at], table_ref[1, at]
                value = own[step][:, half * block : (half + 1) * block].astype(F32)
                out_ref[group, :, pl.ds(pl.multiple_of(slot * block, block), block)] = (
                    value * scale * gain_ref[source]
                ).astype(BF)


def norm_pieces(pieces, gain, table, count):
    rows, width = pieces[0].shape
    groups = len(pieces) // count
    rows_at = min(256, rows)
    blocks = table.shape[1]
    gains = gain.reshape(blocks, 1, count * width // blocks)
    out = pl.pallas_call(
        functools.partial(norm_kernel, count),
        grid=(rows // rows_at,),
        in_specs=[
            pl.BlockSpec(memory_space=pltpu.SMEM),
            pl.BlockSpec(gains.shape, lambda i: (0, 0, 0)),
        ]
        + [pl.BlockSpec((rows_at, width), lambda i: (i, 0))] * len(pieces),
        out_specs=pl.BlockSpec((groups, rows_at, count * width), lambda i: (0, i, 0)),
        out_shape=jax.ShapeDtypeStruct((groups, rows, count * width), BF),
        compiler_params=params("arbitrary"),
        name="norm_pieces",
    )(table, gains, *pieces)
    return out.reshape(groups * rows, count * width)


def recurrence_kernel(
    sequences, projected_ref, taps_ref, recur_ref, inject_ref, decay_ref, token_ref, out_ref, filter_ref, state_ref, a_ref, b_ref
):
    rows, channels = out_ref.shape
    taps = taps_ref.shape[0]
    history = (taps - 1) * sequences

    @pl.when(pl.program_id(1) == 0)
    def _():
        filter_ref[0:history, :] = jnp.zeros((history, channels), F32)
        state_ref[...] = jnp.zeros_like(state_ref)

    projected = projected_ref[...]
    gate = projected[:, :channels]
    filter_ref[history : history + rows, :] = projected[:, channels:].astype(BF).astype(F32)
    summed = taps_ref[0:1, :] * filter_ref[0:rows, :]
    for k in range(1, taps):
        summed = summed + taps_ref[k : k + 1, :] * filter_ref[k * sequences : k * sequences + rows, :]
    filter_ref[0:history, :] = filter_ref[rows : rows + history, :]
    mixed = summed.astype(BF)
    recur = jax.nn.sigmoid(jnp.dot(mixed, recur_ref[...], preferred_element_type=F32))
    inject = jax.nn.sigmoid(jnp.dot(mixed, inject_ref[...], preferred_element_type=F32))
    log_decay = decay_ref[...] * recur + token_ref[:, 0:1]
    decay = jnp.exp(log_decay)
    square = log_decay * log_decay
    small = log_decay * (
        1.0 - square * (1.0 / 3.0 - square * (2.0 / 15.0 - square * (17.0 / 315.0 - square * (62.0 / 2835.0))))
    )
    tangent = jnp.where(log_decay > -0.125, small, jnp.tanh(log_decay))
    a_ref[...] = decay
    b_ref[...] = jnp.sqrt(-tangent * (1.0 + decay * decay)) * (inject * mixed.astype(F32))
    state = state_ref[...]
    for step in range(rows // sequences):
        at = slice(step * sequences, (step + 1) * sequences)
        state = a_ref[at, :] * state + b_ref[at, :]
        b_ref[at, :] = state
    state_ref[...] = state
    out_ref[...] = (b_ref[...] * jax.nn.gelu(gate)).astype(BF)


def recurrence(projected, taps, recur, inject, decay, token_decay, sequences):
    rows, doubled = projected.shape
    channels = doubled // 2
    per = sequences * LEN
    block = sequences * 32
    steps = per // block
    return pl.pallas_call(
        functools.partial(recurrence_kernel, sequences),
        grid=(rows // per, steps),
        in_specs=[
            pl.BlockSpec((block, doubled), lambda g, i: (g * steps + i, 0)),
            pl.BlockSpec(taps.shape, lambda g, i: (0, 0)),
            pl.BlockSpec(recur.shape, lambda g, i: (0, 0)),
            pl.BlockSpec(inject.shape, lambda g, i: (0, 0)),
            pl.BlockSpec((1, channels), lambda g, i: (0, 0)),
            pl.BlockSpec((block, token_decay.shape[1]), lambda g, i: (g * steps + i, 0)),
        ],
        out_specs=pl.BlockSpec((block, channels), lambda g, i: (g * steps + i, 0)),
        out_shape=jax.ShapeDtypeStruct((rows, channels), BF),
        scratch_shapes=[
            pltpu.VMEM((block + (taps.shape[0] - 1) * sequences, channels), F32),
            pltpu.VMEM((sequences, channels), F32),
            pltpu.VMEM((block, channels), F32),
            pltpu.VMEM((block, channels), F32),
        ],
        compiler_params=params("arbitrary", "arbitrary"),
        name="recurrence",
    )(projected, taps, recur, inject, decay, token_decay)


def time_major(rows_first, sequences):
    rows, width = rows_first.shape
    return rows_first.reshape(sequences, rows // sequences, width).swapaxes(0, 1).reshape(rows, width)


def sequence_major(time_first, sequences):
    rows, width = time_first.shape
    return time_first.reshape(rows // sequences, sequences, width).swapaxes(0, 1).reshape(rows, width)


def decay_columns(token_log_decay, sequences):
    ordered = token_log_decay.reshape(sequences, LEN).T.reshape(-1, 1)
    return jnp.broadcast_to(ordered, (ordered.shape[0], 128))


def block_dense(weight):
    groups, block_width, _ = weight.shape
    identity = jnp.eye(groups, dtype=BF)[:, None, :, None]
    return (weight[:, :, None, :] * identity).reshape(groups * block_width, groups * block_width)


def product(left, right):
    return jnp.dot(left, right, preferred_element_type=F32)


def plain_shards(
    tokens,
    recurrence_norm_gain,
    output_gate_weight,
    recurrence_input_weight,
    convolution_taps,
    recurrence_gate_weight,
    input_gate_weight,
    base_decay_logit,
    token_log_decay,
    recurrence_output_weight,
    feedforward_norm_gain,
    feedforward_gate_weight,
    feedforward_up_weight,
    feedforward_down_weight,
):
    sequences = tokens.shape[0] // LEN

    def rows_of(weight):
        return lax.all_gather(weight, "fs", axis=0, tiled=True)

    def columns_of(weight):
        return lax.all_gather(weight, "fs", axis=1, tiled=True)

    def normed_of(own, gain):
        widened = lax.all_gather(own, "tp", axis=1, tiled=True).astype(F32)
        scale = lax.rsqrt(jnp.mean(widened * widened, axis=-1, keepdims=True) + EPSILON)
        return (widened * scale * gain).astype(BF)

    def scattered(term):
        return lax.psum_scatter(term.astype(BF), "tp", scatter_dimension=1, tiled=True).astype(F32)

    ordered = time_major(tokens, sequences)
    normed = normed_of(ordered, recurrence_norm_gain)
    projected = jnp.concatenate(
        [product(normed, rows_of(output_gate_weight)), product(normed, rows_of(recurrence_input_weight))], axis=1
    )
    carried = recurrence(
        projected,
        convolution_taps,
        block_dense(recurrence_gate_weight),
        block_dense(input_gate_weight),
        -GATE_EXPONENT * jax.nn.softplus(-base_decay_logit)[None, :],
        decay_columns(token_log_decay, sequences),
        sequences,
    )
    mixed = scattered(product(carried, columns_of(recurrence_output_weight)))
    residual = sequence_major((ordered.astype(F32) + mixed).astype(BF), sequences)
    normed_two = normed_of(residual, feedforward_norm_gain)
    gate_hidden = product(normed_two, rows_of(feedforward_gate_weight))
    up_hidden = product(normed_two, rows_of(feedforward_up_weight))
    hidden = (jax.nn.silu(gate_hidden) * up_hidden).astype(BF)
    down = scattered(product(hidden, columns_of(feedforward_down_weight)))
    return (residual.astype(F32) + down).astype(BF)


def paired_shards(
    tokens,
    recurrence_norm_gain,
    output_gate_weight,
    recurrence_input_weight,
    convolution_taps,
    recurrence_gate_weight,
    input_gate_weight,
    base_decay_logit,
    token_log_decay,
    recurrence_output_weight,
    feedforward_norm_gain,
    feedforward_gate_weight,
    feedforward_up_weight,
    feedforward_down_weight,
):
    fs, tp = lax.axis_size("fs"), lax.axis_size("tp")
    lines = fs // 2
    at_fs, place = lax.axis_index("fs"), lax.axis_index("tp")
    side, level = at_fs % 2, at_fs // 2
    first = side == 0
    rows = tokens.shape[0]
    half = rows // 2
    sequences = rows // LEN
    groups = [[way + 2 * i for i in range(lines)] for way in range(2)]

    def over_x(value):
        return lax.ppermute(value, "fs", [(i, i ^ 1) for i in range(fs)])

    def over_z(value):
        return lax.ppermute(value, "fs", [(i, (i + 2) % fs) for i in range(fs)])

    def over_tp(value, bit):
        return lax.ppermute(value, "tp", [(i, i ^ bit) for i in range(tp)])

    def after(value, *earlier):
        return lax.optimization_barrier((value, *earlier))[0]

    def halves(weight, axis):
        low, high = jnp.split(weight, 2, axis=axis)
        return jnp.where(first, low, high), jnp.where(first, high, low)

    def in_order(own, other):
        return jnp.where(first, jnp.stack([own, other]), jnp.stack([other, own]))

    def gathered(pair):
        return lax.all_gather(pair, "fs", axis=0, tiled=True, axis_index_groups=groups)

    def spread(own, *first_ready):
        over, across = over_x(own), over_tp(own, 2)
        corner_y = over_tp(over[:half], 2)
        corner_x = over_x(after(across[half:], *first_ready))
        corner = jnp.concatenate([corner_y, corner_x])
        return [
            own, over_tp(own, 1), across, over_tp(across, 1),
            over, over_tp(over, 1), corner, over_tp(corner, 1),
        ]

    def summed_to_owner(values, columns):
        theirs, mine = values[rows:], values[:rows]

        def part(of, step):
            return product(of, columns(step)).astype(BF)

        def add(*terms):
            total = terms[0].astype(F32)
            for term in terms[1:]:
                total = total + term.astype(F32)
            return total

        swapped = over_tp(part(theirs, 3), 1)
        corner_own = part(theirs, 2)
        mine = after(mine, corner_own)
        corner = add(corner_own, swapped).astype(BF)
        by_x, by_y = over_x(corner[:half]), over_tp(corner[half:], 2)
        far_swapped = over_tp(part(mine, 3), 1)
        near_swapped = over_tp(part(theirs, 1), 1)
        far, near = part(mine, 2), part(theirs, 0)
        y_late_term = add(far[half:], far_swapped[half:]).astype(BF)
        x_early_term = add(near[:half], near_swapped[:half]).astype(BF)
        y_late, x_early = over_tp(y_late_term, 2), over_x(x_early_term)
        far, far_swapped, near, near_swapped, mine = lax.optimization_barrier(
            (far, far_swapped, near, near_swapped, mine, y_late_term, x_early_term)
        )[:5]
        own_swapped = over_tp(part(mine, 1), 1)
        own = add(part(mine, 0), own_swapped)
        y_early = over_tp(add(far[:half], far_swapped[:half], by_x).astype(BF), 2)
        x_late = over_x(add(near[half:], near_swapped[half:], by_y).astype(BF))
        return jnp.concatenate([add(own[:half], y_early, x_early), add(own[half:], y_late, x_late)], axis=0)

    steps = jnp.arange(fs, dtype=jnp.int32)
    source = ((steps // 2) ^ place) * 2 + steps % 2
    in_line = jnp.stack([source, source])

    gate_own, gate_other = halves(output_gate_weight, 1)
    in_own, in_other = halves(recurrence_input_weight, 1)
    project_pair = in_order(jnp.concatenate([gate_own, in_own], 1), over_x(jnp.concatenate([gate_other, in_other], 1)))
    project_weight = gathered(project_pair)
    project_weight = project_weight.reshape(-1, project_weight.shape[-1])
    out_own, out_other = halves(recurrence_output_weight, 0)
    out_ring = [jnp.stack([out_own, over_x(out_other)])]
    for _ in range(1, lines):
        out_ring.append(over_z(out_ring[-1]))
    out_weight = jnp.stack(out_ring)

    ffn_gate_own, ffn_gate_other = halves(feedforward_gate_weight, 1)
    ffn_up_own, ffn_up_other = halves(feedforward_up_weight, 1)
    ffn_pair = in_order(
        jnp.concatenate([ffn_gate_own, ffn_up_own], 1),
        over_x(jnp.concatenate([ffn_gate_other, ffn_up_other], 1)),
    )
    ffn_weight = gathered(ffn_pair)
    ffn_weight = ffn_weight.reshape(-1, ffn_weight.shape[-1])

    down_own, down_other = halves(feedforward_down_weight, 0)
    down_pair = in_order(down_own, over_x(down_other))
    down_weight = gathered(down_pair)

    ordered = time_major(tokens, sequences)
    pieces = spread(ordered, ffn_pair)
    normed = norm_pieces(pieces, recurrence_norm_gain, in_line, tp)
    projected = product(normed, project_weight)

    def out_columns(step):
        pair = lax.dynamic_index_in_dim(out_weight, (level - (place ^ step)) % lines, axis=0, keepdims=False)
        return jnp.where(first, jnp.concatenate([pair[0], pair[1]], 1), jnp.concatenate([pair[1], pair[0]], 1))

    def down_columns(step):
        pair = lax.dynamic_slice_in_dim(down_weight, (place ^ step) * 2, 2, axis=0)
        return jnp.concatenate([pair[0], pair[1]], 1)

    token_decay = token_log_decay.reshape(sequences, LEN)
    token_columns = jnp.concatenate(
        [decay_columns(token_decay, sequences), decay_columns(over_x(token_decay), sequences)], axis=0
    )
    carried = recurrence(
        projected,
        halves(convolution_taps, 1)[0],
        block_dense(halves(recurrence_gate_weight, 0)[0]),
        block_dense(halves(input_gate_weight, 0)[0]),
        -GATE_EXPONENT * jax.nn.softplus(-halves(base_decay_logit, 0)[0])[None, :],
        token_columns,
        sequences,
    )
    mixed = summed_to_owner(carried, out_columns)
    residual = sequence_major((ordered.astype(F32) + mixed).astype(BF), sequences)
    normed_two = norm_pieces(spread(residual), feedforward_norm_gain, in_line, tp)
    width = ffn_gate_own.shape[1]
    gate_hidden = product(normed_two, ffn_weight[:, :width])
    up_hidden = product(normed_two, ffn_weight[:, width:])
    hidden = (jax.nn.silu(gate_hidden) * up_hidden).astype(BF)
    down = summed_to_owner(hidden, down_columns)
    return (residual.astype(F32) + down).astype(BF)


def pairable(fs, tp):
    return fs == 2 * tp and tp == 4


def solution(mesh):
    in_specs = (
        P("fs", "tp"), P(), P("fs", "tp"), P("fs", "tp"), P(None, "tp"), P("tp", None, None), P("tp", None, None),
        P("tp"), P("fs"), P("tp", "fs"), P(), P("fs", "tp"), P("fs", "tp"), P("tp", "fs"),
    )
    fs, tp = mesh.shape["fs"], mesh.shape["tp"]

    def whole(*args):
        blocks = args[5].shape[0] // tp
        paired = pairable(fs, tp) and blocks % 2 == 0
        body = paired_shards if paired else plain_shards

        return jax.shard_map(body, mesh=mesh, in_specs=in_specs, out_specs=P("fs", "tp"), check_vma=False)(*args)

    return whole
```
